32 devices in a mesh: ep: 8 (over z, y), tp: 4 (over x, core).
Axes of the slice: x: 2, y: 2, z: 4, core: 2. Of those that a mesh axis runs over, the one named last changes fastest.
Arguments:
- mixer_input: bfloat16 [4096, 2048], P('ep'), may hold values from -6 to 6
- log_forget_total: float32 [16, 4096], P('tp'), may hold values from -684 to 0, as said below
- mixer_gain: float32 [2048], replicated, may hold values from 0.1 to 1.9
- w_query: bfloat16 [2048, 1024], P(None, 'tp'), may hold values from -1 to 1
- w_key: bfloat16 [2048, 256], P(None, 'tp'), may hold values from -8 to 8
- w_value: bfloat16 [2048, 256], P(None, 'tp'), may hold values from -0.125 to 0.125
- w_output: bfloat16 [1024, 2048], replicated, may hold values from -0.1875 to 0.1875
- mixer_post_gain: float32 [2048], replicated, may hold values from 0.1 to 1.9
- expert_input: bfloat16 [2048, 2048], P('ep'), may hold values from -6 to 6
- expert_ids: int32 [2048, 2], P('ep'), may hold values from 0 to 7, all different within a row; in each aligned block of 64 rows (0 to 63, 64 to 127, ...) at most 32 rows name the same one
- route_weight: float32 [2048, 2], P('ep'), may hold values from 0.1 to 1
- expert_gain: float32 [2048], replicated, may hold values from 0.1 to 1.9
- w_gate: bfloat16 [8, 2048, 3584], P('ep', None, 'tp'), may hold values from -0.125 to 0.125
- w_up: bfloat16 [8, 2048, 3584], P('ep', None, 'tp'), may hold values from -0.125 to 0.125
- w_down: bfloat16 [8, 3584, 2048], P('ep', 'tp'), may hold values from -0.09375 to 0.09375
- expert_post_gain: float32 [2048], replicated, may hold values from 0.1 to 1.9
Outputs:
- mixer_out: bfloat16 [4096, 2048], P(('ep', 'tp'))
- expert_out: bfloat16 [2048, 2048], P(('ep', 'tp'))
The draws below stay inside these ranges and needn't reach their ends.
Inputs may be any that keep to these rules, and one draw needn't show every extreme that they name: `expert_ids`: in each aligned block of 64 tokens no expert is named by more than 32 of them. `log_forget_total`: each head's values never rise along the positions.
All inputs are finite; a program needn't handle non-finite values.
Results may differ from the reference program's by a relative error of at most 0.012.
The reference program's roundings to bfloat16 on the way count: a program that leaves them out, or rounds other values in their place, can miss the bound.
Values may be sent and summed in bfloat16 or wider, within the bound.
A program may use at most 128 MiB of HBM per device.

```python
import math
import jax
import jax.numpy as jnp
import numpy as np
from jax import lax

D = 2048
QUERY_HEADS = 16
KV_HEADS = 4
HD = 64
FF = 3584
TOP_K = 2
ATT_ROWS = 512
ATTENTION_SPAN = 4096
MOE_TOKENS = 2048
EXPERTS = 8
QROWS = 64
CAPQ = 32
N_EP = 8
N_TP = 4


def draw_mixer_input(key, part):
    drawn = jax.random.normal(jax.random.fold_in(key, 7), (ATTENTION_SPAN, D), jnp.float32)
    return jnp.clip(drawn, -6.0, 6.0).astype(jnp.bfloat16)


def draw_log_forget_total(key, part):
    order = jax.random.permutation(jax.random.fold_in(key, 21), QUERY_HEADS)
    slow_count = QUERY_HEADS // 2
    slow = order < slow_count
    slow_rate = jax.random.uniform(jax.random.fold_in(key, 22), (QUERY_HEADS,), jnp.float32, 0.2, 0.8) / ATTENTION_SPAN
    fast_rate = 1.0 / jax.random.uniform(jax.random.fold_in(key, 23), (QUERY_HEADS,), jnp.float32, 30.0, 100.0)
    step_rate = jnp.where(slow, slow_rate, fast_rate)
    block_factor = jnp.exp(jax.random.uniform(jax.random.fold_in(key, 24), (ATTENTION_SPAN // ATT_ROWS, QUERY_HEADS), jnp.float32, math.log(0.4), math.log(2.5)))
    per_position = jnp.repeat(block_factor, ATT_ROWS, axis=0)
    rough = jax.random.uniform(jax.random.fold_in(key, 25), (ATTENTION_SPAN, QUERY_HEADS), jnp.float32, 0.3, 1.7)
    gate_logarithm = -step_rate[None, :] * per_position * rough
    spike_position = jax.random.randint(jax.random.fold_in(key, 26), (3,), 0, ATTENTION_SPAN)
    spike_length = jnp.log(jax.random.uniform(jax.random.fold_in(key, 27), (3, QUERY_HEADS), jnp.float32, 0.6, 0.8))
    match_count = (jnp.arange(ATTENTION_SPAN)[:, None] == spike_position[None, :]).astype(jnp.float32)
    gate_logarithm = gate_logarithm + jnp.sum(match_count[:, :, None] * spike_length[None, :, :], axis=1)
    return jnp.transpose(jnp.cumsum(gate_logarithm, axis=0))


def query_key_pair(key):
    query_w = jax.random.normal(jax.random.fold_in(key, 31), (D, QUERY_HEADS * HD), jnp.float32) * D ** (-0.5)
    key_w = jax.random.normal(jax.random.fold_in(key, 32), (D, KV_HEADS * HD), jnp.float32) * D ** (-0.5)
    return (jnp.clip(query_w, -1.0, 1.0), jnp.clip(key_w, -8.0, 8.0))


def draw_w_query(key, part):
    return query_key_pair(key)[0].astype(jnp.bfloat16)


def draw_w_key(key, part):
    return query_key_pair(key)[1].astype(jnp.bfloat16)


def level_of(key, extent, split, smallest, top_value):
    def one(axis_at, parts):
        heights = jax.random.uniform(jax.random.fold_in(jax.random.fold_in(key, 6), axis_at), (parts,), jnp.float32, smallest / len(split), top_value / len(split))
        return jnp.repeat(jnp.exp(heights), extent[axis_at] // parts).reshape((-1,) + (1,) * (len(extent) - axis_at - 1))

    loudness = one(*split[0])
    for cut in split[1:]:
        loudness = loudness * one(*cut)
    return loudness


def deal_out(rng, own, number, rows, number_of, top, bound, skew):
    order = jax.random.permutation(rng, number_of)
    heavy_load, usual = portions_of(number_of, rows * top, bound, skew, True), portions_of(number_of, rows * top, bound, skew, False)
    places = jnp.arange(number_of)

    def named(tallies, turn):
        used = int((tallies > 0).sum())
        fixed = max(1, used // 4)
        moved = fixed + (places - fixed + turn * (used - fixed)) % max(1, number_of - fixed)
        return jnp.zeros((number_of,), jnp.int32).at[order[jnp.where(places < fixed, places, moved)]].set(jnp.asarray(tallies, jnp.int32))

    tallies = jnp.where(number % 4 == 0, named(heavy_load, number // 4), named(usual, number - number // 4 - 1))
    mixed = jax.random.permutation(jax.random.fold_in(own, 3), number_of)
    source_of, receiver = mixed[0:number_of // 2 * 2:2], mixed[1:number_of // 2 * 2:2]
    margin = jnp.minimum(tallies[source_of] - 1, bound - tallies[receiver]) // 2
    margin = jnp.where((source_of == order[0]) | (receiver == order[0]) | (tallies[receiver] == 0), 0, jnp.maximum(margin, 0))
    moved = jax.random.randint(jax.random.fold_in(own, 4), (number_of // 2,), 0, 1 << 20) % (margin + 1)
    tallies = tallies.at[source_of].add(-moved).at[receiver].add(moved)
    items = jnp.searchsorted(jnp.cumsum(tallies), jnp.arange(rows * top), side="right").astype(jnp.int32)
    listing = items.reshape(top, rows).T
    listing = listing[jax.random.permutation(jax.random.fold_in(own, 1), rows)]
    turn = jax.random.randint(jax.random.fold_in(own, 2), (rows, 1), 0, top)
    return jnp.take_along_axis(listing, (jnp.arange(top)[None, :] + turn) % top, axis=1)


def portions_of(amount, total, reach, slope, full):
    weights = [(1 << 20) // math.isqrt(rank ** slope) + 1 for rank in range(1, amount + 1)]
    largest = reach if full else min(reach, max(-(-total // amount), total * weights[0] // sum(weights)))
    least = 1 if total - largest >= amount - 1 else 0
    counts, rest = [largest] + [least] * (amount - 1), total - largest - least * (amount - 1)
    while rest > 0:
        candidates = [i for i in range(1, amount) if counts[i] < largest] or [i for i in range(1, amount) if counts[i] < reach]
        mass, left = sum([weights[i] for i in candidates]), rest
        for i in candidates:
            addition = min(reach - counts[i], max(1, left * weights[i] // mass), rest)
            counts[i] = counts[i] + addition
            rest = rest - addition
    return np.array(counts)


def scatter_about(own_key, shape, scale, reach, split=(), held_as=jnp.bfloat16):
    gain = level_of(own_key, shape, split, -0.22, 0.18) if split else 1.0
    entries = jax.random.normal(own_key, shape, jnp.float32) * scale * gain
    return jnp.minimum(jnp.maximum(entries, -reach), reach).astype(held_as)


def setup_inputs(seed: int = 0) -> dict:
    seeds = jax.random.split(jax.random.key(seed), 17)
    mixer_input = draw_mixer_input(jax.random.fold_in(seeds[16], 71), 0)
    log_forget_total = draw_log_forget_total(jax.random.fold_in(seeds[16], 71), 0)
    mixer_gain = jnp.clip(1.0 + 0.18 * jax.random.normal(seeds[2], (D,), jnp.float32), 0.1, 1.9)
    w_query = draw_w_query(jax.random.fold_in(seeds[16], 71), 0)
    w_key = draw_w_key(jax.random.fold_in(seeds[16], 71), 0)
    w_value = scatter_about(seeds[5], (D, KV_HEADS * HD), D ** -0.5, 0.125, ((1, 4),))
    w_output = scatter_about(seeds[6], (QUERY_HEADS * HD, D), (QUERY_HEADS * HD) ** -0.5, 0.1875)
    mixer_post_gain = jnp.clip(1.0 + 0.18 * jax.random.normal(seeds[7], (D,), jnp.float32), 0.1, 1.9)
    expert_input = scatter_about(seeds[8], (MOE_TOKENS, D), 1.0, 6.0, ((0, 8),))
    expert_ids_keys = jax.random.split(jax.random.fold_in(seeds[9], 1), MOE_TOKENS // QROWS)
    expert_ids_turns = jax.random.permutation(jax.random.fold_in(seeds[9], 3), MOE_TOKENS // QROWS)
    expert_ids = jax.vmap(lambda own, number: deal_out(jax.random.fold_in(seeds[9], 2), own, number, QROWS, EXPERTS, TOP_K, CAPQ, 2))(expert_ids_keys, expert_ids_turns).reshape((MOE_TOKENS, TOP_K))
    route_weight = jnp.clip(jnp.exp(math.log(1.0) - 2.3025851 * jax.random.uniform(seeds[10], (MOE_TOKENS, TOP_K), jnp.float32) ** level_of(seeds[10], (MOE_TOKENS, TOP_K), ((0, 8),), -0.2, 0.2)), 0.1, 1.0)
    expert_gain = jnp.clip(1.0 + 0.18 * jax.random.normal(seeds[11], (D,), jnp.float32), 0.1, 1.9)
    w_gate = scatter_about(seeds[12], (EXPERTS, D, FF), D ** -0.5, 0.125, ((0, 8), (2, 4)))
    w_up = scatter_about(seeds[13], (EXPERTS, D, FF), D ** -0.5, 0.125, ((0, 8), (2, 4)))
    w_down = scatter_about(seeds[14], (EXPERTS, FF, D), FF ** -0.5, 0.09375, ((0, 8), (1, 4)))
    expert_post_gain = jnp.clip(1.0 + 0.18 * jax.random.normal(seeds[15], (D,), jnp.float32), 0.1, 1.9)
    return {"mixer_input": mixer_input, "log_forget_total": log_forget_total, "mixer_gain": mixer_gain, "w_query": w_query, "w_key": w_key, "w_value": w_value, "w_output": w_output, "mixer_post_gain": mixer_post_gain, "expert_input": expert_input, "expert_ids": expert_ids, "route_weight": route_weight, "expert_gain": expert_gain, "w_gate": w_gate, "w_up": w_up, "w_down": w_down, "expert_post_gain": expert_post_gain}


NEG_FILL = -1e+30
NORM_EPS = 1e-06

def norm_rows(values_in, gain_vec):
    widened = values_in.astype(jnp.float32)
    return widened * lax.rsqrt(lax.optimization_barrier(jnp.mean(widened * widened, axis=-1, keepdims=True)) + NORM_EPS) * gain_vec.astype(jnp.float32)

def rounded(values_in):
    return lax.optimization_barrier(values_in.astype(jnp.bfloat16))

def mixer_part(mixer_input, log_forget_total, mixer_gain, w_query, w_key, w_value, w_output, mixer_post_gain):
    normed = rounded(norm_rows(mixer_input, mixer_gain))
    queries = rounded(jnp.dot(normed, w_query, preferred_element_type=jnp.float32))
    key_rows = rounded(jnp.dot(normed, w_key, preferred_element_type=jnp.float32))
    value_rows = rounded(jnp.dot(normed, w_value, preferred_element_type=jnp.float32))
    group_size = QUERY_HEADS // KV_HEADS
    block_rows = math.gcd(ATTENTION_SPAN, 512)
    block_total = ATTENTION_SPAN // block_rows
    query_blocks = queries.reshape(block_total, block_rows, KV_HEADS, group_size, HD)
    key_wide = key_rows.astype(jnp.float32).reshape(ATTENTION_SPAN, KV_HEADS, HD)
    value_wide = value_rows.astype(jnp.float32).reshape(ATTENTION_SPAN, KV_HEADS, HD)
    gate_totals = log_forget_total.astype(jnp.float32).reshape(KV_HEADS, group_size, ATTENTION_SPAN)
    positions = jnp.arange(ATTENTION_SPAN, dtype=jnp.int32)
    score_scale = HD ** (-0.5)

    def one_block(operands):
        query_block, block_index = operands
        first_row = (block_index * block_rows).astype(jnp.int32)
        query_pos = first_row + jnp.arange(block_rows, dtype=jnp.int32)
        visible = positions[None, :] <= query_pos[:, None]
        outputs = []
        for head_group in range(KV_HEADS):
            group_gates = gate_totals[head_group]
            query_gate = lax.dynamic_slice_in_dim(group_gates, first_row, block_rows, 1)
            scores = jnp.einsum('qjd,kd->jqk', query_block[:, head_group].astype(jnp.float32), key_wide[:, head_group]) * score_scale
            scores = scores + query_gate[:, :, None] - group_gates[:, None, :]
            scores = jnp.where(visible[None], scores, NEG_FILL)
            row_max = lax.optimization_barrier(jnp.max(scores, axis=-1, keepdims=True))
            shifted = jnp.where(visible[None], jnp.exp(scores - row_max), 0.0)
            denominator = lax.optimization_barrier(jnp.sum(shifted, axis=-1))
            weights = rounded(shifted).astype(jnp.float32)
            numerator = jnp.einsum('jqk,kd->qjd', weights, value_wide[:, head_group])
            outputs.append(numerator / jnp.transpose(denominator)[:, :, None])
        return rounded(jnp.concatenate(outputs, axis=1).reshape(block_rows, QUERY_HEADS * HD))
    mixed_heads = lax.map(one_block, (query_blocks, jnp.arange(block_total, dtype=jnp.int32)))
    mixed_heads = mixed_heads.reshape(ATTENTION_SPAN, QUERY_HEADS * HD)
    projected = jnp.dot(mixed_heads, w_output, preferred_element_type=jnp.float32)
    return norm_rows(projected, mixer_post_gain).astype(jnp.bfloat16)

def expert_part(expert_input, expert_ids, route_weight, expert_gain, w_gate, w_up, w_down, expert_post_gain):
    normed = rounded(norm_rows(expert_input, expert_gain))
    assigned = MOE_TOKENS * TOP_K
    capacity = N_EP * N_TP * CAPQ
    group_units = FF // N_TP
    flat_ids = expert_ids.reshape(assigned)
    owners = jnp.concatenate([jnp.arange(assigned, dtype=jnp.int32) // TOP_K, jnp.full((1,), MOE_TOKENS, jnp.int32)])
    shares = jnp.concatenate([route_weight.reshape(assigned).astype(jnp.float32), jnp.zeros((1,), jnp.float32)])
    padded_rows = jnp.concatenate([normed, jnp.zeros((1, D), jnp.bfloat16)], axis=0)

    def one_expert(running, expert):
        chosen = flat_ids == expert
        slot_ranks = jnp.cumsum(chosen.astype(jnp.int32)) - 1
        slot_target = jnp.where(chosen, slot_ranks, capacity).astype(jnp.int32)
        slot_table = jnp.full((capacity,), assigned, jnp.int32).at[slot_target].set(jnp.arange(assigned, dtype=jnp.int32), mode='drop')
        token_rows = owners[slot_table]
        inputs = padded_rows[token_rows]
        gate_part = jnp.dot(inputs, w_gate[expert], preferred_element_type=jnp.float32)
        up_part = jnp.dot(inputs, w_up[expert], preferred_element_type=jnp.float32)
        hidden = rounded(jax.nn.silu(gate_part) * up_part)
        down_local = w_down[expert]
        summed = jnp.zeros((capacity, D), jnp.float32)
        for group_index in range(N_TP):
            low_unit = group_index * group_units
            group_term = jnp.dot(hidden[:, low_unit:low_unit + group_units], down_local[low_unit:low_unit + group_units], preferred_element_type=jnp.float32)
            summed = summed + rounded(group_term).astype(jnp.float32)
        expert_rows = rounded(summed).astype(jnp.float32)
        running = running.at[token_rows].add(shares[slot_table][:, None] * expert_rows, mode='drop')
        return (running, None)
    combined, _ = lax.scan(one_expert, jnp.zeros((MOE_TOKENS, D), jnp.float32), jnp.arange(EXPERTS, dtype=jnp.int32))
    return norm_rows(combined, expert_post_gain).astype(jnp.bfloat16)

def reference(mixer_input, log_forget_total, mixer_gain, w_query, w_key, w_value, w_output, mixer_post_gain, expert_input, expert_ids, route_weight, expert_gain, w_gate, w_up, w_down, expert_post_gain):
    mixer_out = mixer_part(mixer_input, log_forget_total, mixer_gain, w_query, w_key, w_value, w_output, mixer_post_gain)
    expert_out = expert_part(expert_input, expert_ids, route_weight, expert_gain, w_gate, w_up, w_down, expert_post_gain)
    return (mixer_out, expert_out)
```

```python
import functools

import jax
import jax.numpy as jnp
from jax import lax
from jax.experimental import pallas as pl
from jax.experimental.pallas import tpu as pltpu
from jax.sharding import PartitionSpec as P

HD = 64
TOP_K = 2


NEG_FILL = -1e30
NORM_EPS = 1e-06


def norm_rows(values_in, gain_vec):
    widened = values_in.astype(jnp.float32)
    return (
        widened
        * lax.rsqrt(jnp.mean(widened * widened, axis=-1, keepdims=True) + NORM_EPS)
        * gain_vec
    )


def attention_kernel(rows, heads, q_ref, kv_ref, gate_ref, out_ref, max_ref, acc_ref):
    own = lax.axis_index("ep")
    max_ref[...] = jnp.full(max_ref.shape, NEG_FILL, jnp.float32)
    acc_ref[...] = jnp.zeros(acc_ref.shape, jnp.float32)

    def block(index, diagonal):
        first = pl.multiple_of(index * rows, rows)
        kv = kv_ref[pl.ds(first, rows), :]
        keys = kv[:, :HD]
        lane = lax.broadcasted_iota(jnp.int32, kv.shape, 1)
        values = jnp.where(lane < HD, jnp.ones_like(kv), kv)
        gates = gate_ref[:, pl.ds(first, rows)]
        for head in range(heads):
            scores = lax.dot_general(
                q_ref[head], keys, (((1,), (1,)), ((), ())), preferred_element_type=jnp.float32
            )
            scores = scores - gates[head : head + 1, :]
            if diagonal:
                row = lax.broadcasted_iota(jnp.int32, scores.shape, 0)
                column = lax.broadcasted_iota(jnp.int32, scores.shape, 1)
                scores = jnp.where(column <= row, scores, NEG_FILL)
            old_max = max_ref[head][:, :1]
            new_max = jnp.maximum(old_max, jnp.max(scores, axis=1, keepdims=True))
            shifted = jnp.exp(scores - new_max).astype(jnp.bfloat16)
            acc_ref[head] = acc_ref[head] * jnp.exp(old_max - new_max) + jnp.dot(
                shifted, values, preferred_element_type=jnp.float32
            )
            max_ref[head] = jnp.broadcast_to(new_max, max_ref.shape[1:])

    def earlier(index, carry):
        block(index, False)
        return carry

    lax.fori_loop(0, own, earlier, 0)
    block(own, True)
    for head in range(heads):
        total = acc_ref[head]
        out_ref[head] = (total[:, HD:] / total[:, :HD]).astype(out_ref.dtype)


def attend(queries, kv_rows, gate_totals):
    heads, rows, _ = queries.shape
    return pl.pallas_call(
        functools.partial(attention_kernel, rows, heads),
        out_shape=jax.ShapeDtypeStruct(queries.shape, jnp.bfloat16),
        in_specs=[pl.BlockSpec(memory_space=pltpu.VMEM)] * 3,
        out_specs=pl.BlockSpec(memory_space=pltpu.VMEM),
        scratch_shapes=[
            pltpu.VMEM((heads, rows, 2 * HD), jnp.float32),
            pltpu.VMEM((heads, rows, 2 * HD), jnp.float32),
        ],
        cost_estimate=pl.CostEstimate(
            flops=30_000_000_000, bytes_accessed=4_000_000, transcendentals=0
        ),
        compiler_params=pltpu.CompilerParams(vmem_limit_bytes=32 * 1024 * 1024),
    )(queries, kv_rows, gate_totals)


def mixer_half(
    mixer_input, log_forget_total, mixer_gain, w_query, w_key, w_value, w_output, mixer_post_gain
):
    row_count = mixer_input.shape[0]
    head_local = w_query.shape[1] // HD
    normed = norm_rows(mixer_input, mixer_gain).astype(jnp.bfloat16)
    w_kv = jnp.concatenate([w_key, w_value], axis=1)
    kv_rows = jnp.dot(normed, w_kv, preferred_element_type=jnp.float32).astype(jnp.bfloat16)
    kv_all = lax.all_gather(kv_rows, "ep", axis=0, tiled=True)
    queries = jnp.dot(normed, w_query, preferred_element_type=jnp.float32).astype(jnp.bfloat16)
    queries = queries * jnp.bfloat16(HD ** (-0.5))
    queries = jnp.transpose(queries.reshape(row_count, head_local, HD), (1, 0, 2))
    mixed = attend(queries, kv_all, log_forget_total)
    mixed_heads = jnp.transpose(mixed, (1, 0, 2)).reshape(row_count, head_local * HD)
    by_rows = lax.all_to_all(mixed_heads, "tp", split_axis=0, concat_axis=1, tiled=True)
    projected = jnp.dot(by_rows, w_output, preferred_element_type=jnp.float32)
    return norm_rows(projected, mixer_post_gain).astype(jnp.bfloat16)


def expert_half(
    expert_input, expert_ids, route_weight, expert_gain, w_gate, w_up, w_down, expert_post_gain
):
    row_count = expert_input.shape[0]
    quarters = lax.axis_size("tp")
    experts = lax.axis_size("ep")
    quarter_rows = row_count // quarters
    slot_count = 2 * TOP_K * quarter_rows // experts
    first = lax.axis_index("tp") * quarter_rows
    own_input = lax.dynamic_slice_in_dim(expert_input, first, quarter_rows, 0)
    own_weights = lax.dynamic_slice_in_dim(route_weight, first, quarter_rows, 0)
    routed = lax.dynamic_slice_in_dim(expert_ids, first, quarter_rows, 0)
    normed = norm_rows(own_input, expert_gain).astype(jnp.bfloat16)
    matches = routed[:, :, None] == jnp.arange(experts, dtype=jnp.int32)[None, None, :]
    matches = matches.astype(jnp.bfloat16)
    per_token = jnp.sum(matches, axis=1)
    position = jnp.arange(quarter_rows, dtype=jnp.int32)
    lower = (position[None, :] < position[:, None]).astype(jnp.bfloat16)
    before = jnp.dot(lower, per_token, preferred_element_type=jnp.float32)
    ranks = jnp.sum(matches.astype(jnp.float32) * before[:, None, :], axis=2).astype(jnp.int32)
    slots = routed * slot_count + ranks
    total_slots = experts * slot_count
    chosen = slots[:, :, None] == jnp.arange(total_slots, dtype=jnp.int32)[None, None, :]
    chosen = chosen.astype(jnp.bfloat16)
    outgoing = lax.dot_general(
        jnp.sum(chosen, axis=1), normed, (((0,), (0,)), ((), ())),
        preferred_element_type=jnp.float32,
    ).astype(jnp.bfloat16)
    arrived = lax.all_to_all(
        outgoing.reshape(experts, slot_count, -1), "ep", split_axis=0, concat_axis=0, tiled=True
    )
    flat_rows = lax.all_gather(
        arrived.reshape(total_slots, -1), "tp", axis=0, tiled=True
    )
    gate_part = jnp.dot(flat_rows, w_gate[0], preferred_element_type=jnp.float32)
    up_part = jnp.dot(flat_rows, w_up[0], preferred_element_type=jnp.float32)
    hidden = (jax.nn.silu(gate_part) * up_part).astype(jnp.bfloat16)
    product = jnp.dot(hidden, w_down[0], preferred_element_type=jnp.float32).astype(jnp.bfloat16)
    results = lax.psum_scatter(product, "tp", scatter_dimension=0, tiled=True)
    returned = lax.all_to_all(
        results.reshape(experts, slot_count, -1), "ep", split_axis=0, concat_axis=0, tiled=True
    ).reshape(total_slots, -1)
    combined = 0.0
    for k in range(TOP_K):
        picked = jnp.dot(chosen[:, k], returned, preferred_element_type=jnp.float32)
        combined = combined + own_weights[:, k : k + 1] * picked
    return norm_rows(combined, expert_post_gain).astype(jnp.bfloat16)


def per_device(
    mixer_input,
    log_forget_total,
    mixer_gain,
    w_query,
    w_key,
    w_value,
    w_output,
    mixer_post_gain,
    expert_input,
    expert_ids,
    route_weight,
    expert_gain,
    w_gate,
    w_up,
    w_down,
    expert_post_gain,
):
    mixer_out = mixer_half(
        mixer_input,
        log_forget_total,
        mixer_gain,
        w_query,
        w_key,
        w_value,
        w_output,
        mixer_post_gain,
    )
    expert_out = expert_half(
        expert_input, expert_ids, route_weight, expert_gain, w_gate, w_up, w_down, expert_post_gain
    )
    return (mixer_out, expert_out)


def solution(mesh):
    placed = (
        P("ep", None),
        P("tp", None),
        P(),
        P(None, "tp"),
        P(None, "tp"),
        P(None, "tp"),
        P(),
        P(),
        P("ep", None),
        P("ep", None),
        P("ep", None),
        P(),
        P("ep", None, "tp"),
        P("ep", None, "tp"),
        P("ep", "tp", None),
        P(),
    )
    return jax.shard_map(
        per_device,
        mesh=mesh,
        in_specs=placed,
        out_specs=(P(("ep", "tp"), None), P(("ep", "tp"), None)),
        check_vma=False,
    )
```

```python
import functools

import jax
import jax.numpy as jnp
from jax import lax
from jax.experimental import pallas as pl
from jax.experimental.pallas import tpu as pltpu
from jax.sharding import PartitionSpec as P

HD = 64
TOP_K = 2


NEG_FILL = -1e30
NORM_EPS = 1e-06


def norm_rows(values_in, gain_vec):
    widened = values_in.astype(jnp.float32)
    return (
        widened
        * lax.rsqrt(jnp.mean(widened * widened, axis=-1, keepdims=True) + NORM_EPS)
        * gain_vec
    )


def meet(axis_sizes):
    barrier = pltpu.get_barrier_semaphore()
    for axis, size in axis_sizes:
        place = lax.axis_index(axis)
        for step in range(1, size):
            pl.semaphore_signal(
                barrier,
                inc=1,
                device_id={axis: lax.rem(place + step, size)},
                device_id_type=pl.DeviceIdType.MESH,
            )
    pl.semaphore_wait(barrier, sum(size - 1 for _, size in axis_sizes))


def push(source, target, sems, index, axis, place):
    return pltpu.make_async_remote_copy(
        src_ref=source,
        dst_ref=target,
        send_sem=sems.at[0, index],
        recv_sem=sems.at[1, index],
        device_id={axis: place},
        device_id_type=pl.DeviceIdType.MESH,
    )


def inward_kernel(
    n_ep, rows, heads, q_ref, kv_ref, gate_ref, out_rows, mixed_ref, slots_ref,
    kv_all, max_ref, acc_ref, kv_sem, ep_sem, x_sem, c_sem, d_sem,
):
    own = lax.axis_index("ep")
    quarter = lax.axis_index("tp")
    across = lax.rem(quarter + 2, 4)
    beside = quarter + 1 - 2 * lax.rem(quarter, 2)
    max_ref[...] = jnp.full(max_ref.shape, NEG_FILL, jnp.float32)
    acc_ref[...] = jnp.zeros(acc_ref.shape, jnp.float32)
    meet((("ep", n_ep), ("tp", 4)))

    def block(kv, index, diagonal):
        first = pl.multiple_of(index * rows, rows)
        keys = kv[:, :HD]
        lane = lax.broadcasted_iota(jnp.int32, kv.shape, 1)
        values = jnp.where(lane < HD, jnp.ones_like(kv), kv)
        gates = gate_ref[:, pl.ds(first, rows)]
        for head in range(heads):
            scores = lax.dot_general(
                q_ref[head], keys, (((1,), (1,)), ((), ())), preferred_element_type=jnp.float32
            )
            scores = scores - gates[head : head + 1, :]
            if diagonal:
                row = lax.broadcasted_iota(jnp.int32, scores.shape, 0)
                column = lax.broadcasted_iota(jnp.int32, scores.shape, 1)
                scores = jnp.where(column <= row, scores, NEG_FILL)
            old_max = max_ref[head][:, :1]
            new_max = jnp.maximum(old_max, jnp.max(scores, axis=1, keepdims=True))
            shifted = jnp.exp(scores - new_max).astype(jnp.bfloat16)
            acc_ref[head] = acc_ref[head] * jnp.exp(old_max - new_max) + jnp.dot(
                shifted, values, preferred_element_type=jnp.float32
            )
            max_ref[head] = jnp.broadcast_to(new_max, max_ref.shape[1:])

    def kv_copy(source, place):
        return push(kv_ref, kv_all.at[source], kv_sem, source, "ep", place)

    def ep_copy(source, place):
        return pltpu.make_async_remote_copy(
            src_ref=out_rows.at[place],
            dst_ref=slots_ref.at[quarter, source],
            send_sem=ep_sem.at[0, place],
            recv_sem=ep_sem.at[1, source],
            device_id={"ep": place},
            device_id_type=pl.DeviceIdType.MESH,
        )

    def kv_send(place):
        return pltpu.make_async_remote_copy(
            src_ref=kv_ref,
            dst_ref=kv_all.at[own],
            send_sem=kv_sem.at[0, place],
            recv_sem=kv_sem.at[1, own],
            device_id={"ep": place},
            device_id_type=pl.DeviceIdType.MESH,
        )

    def to_across(source, held):
        return push(held, slots_ref.at[quarter, source], x_sem, source, "tp", across)

    def to_beside(source, held):
        return push(held, slots_ref.at[quarter, source], c_sem, source, "tp", beside)

    def second(source):
        held = slots_ref.at[across, source]
        return push(held, slots_ref.at[across, source], d_sem, source, "tp", beside)

    def send(step, carry):
        @pl.when(own + step < n_ep)
        def _():
            kv_send(own + step).start()

        ep_copy(own, lax.rem(own + step, n_ep)).start()
        return carry

    lax.fori_loop(1, n_ep, send, 0)
    to_across(own, out_rows.at[own]).start()
    to_beside(own, out_rows.at[own]).start()
    slots_ref[quarter, own] = out_rows[own]
    block(kv_ref[...], own, True)

    def work(step, carry):
        @pl.when(step <= own)
        def _():
            kv_copy(own - step, own).wait_recv()
            block(kv_all[own - step], own - step, False)

        source = lax.rem(own - step + n_ep, n_ep)
        ep_copy(source, source).wait_recv()
        held = slots_ref.at[quarter, source]
        to_across(source, held).start()
        to_beside(source, held).start()
        earlier = lax.rem(own - step + 1 + n_ep, n_ep)
        to_across(earlier, slots_ref.at[across, earlier]).wait_recv()
        second(earlier).start()
        return carry

    lax.fori_loop(1, n_ep, work, 0)
    last = lax.rem(own + 1, n_ep)
    to_across(last, slots_ref.at[across, last]).wait_recv()
    second(last).start()
    for head in range(heads):
        total = acc_ref[head]
        mixed_ref[head] = (total[:, HD:] / total[:, :HD]).astype(mixed_ref.dtype)

    def drain(step, carry):
        place = lax.rem(own + step, n_ep)

        @pl.when((step > 0) & (own + step < n_ep))
        def _():
            kv_send(own + step).wait_send()

        @pl.when(step > 0)
        def _():
            ep_copy(own, place).wait_send()

        to_across(place, out_rows.at[own]).wait_send()
        to_beside(place, out_rows.at[own]).wait()
        second(place).wait()
        return carry

    lax.fori_loop(0, n_ep, drain, 0)


def inward(queries, kv_rows, gate_totals, outgoing):
    heads, rows, _ = queries.shape
    n_ep, slot_count, width = outgoing.shape
    pair = pltpu.SemaphoreType.DMA((2, n_ep))
    return pl.pallas_call(
        functools.partial(inward_kernel, n_ep, rows, heads),
        out_shape=(
            jax.ShapeDtypeStruct(queries.shape, jnp.bfloat16),
            jax.ShapeDtypeStruct((4, n_ep, slot_count, width), jnp.bfloat16),
        ),
        in_specs=[pl.BlockSpec(memory_space=pltpu.VMEM)] * 4,
        out_specs=[pl.BlockSpec(memory_space=pltpu.VMEM)] * 2,
        scratch_shapes=[
            pltpu.VMEM((n_ep, rows, 2 * HD), jnp.bfloat16),
            pltpu.VMEM((heads, rows, 2 * HD), jnp.float32),
            pltpu.VMEM((heads, rows, 2 * HD), jnp.float32),
            pair, pair, pair, pair, pair,
        ],
        compiler_params=pltpu.CompilerParams(
            collective_id=0, has_side_effects=True, vmem_limit_bytes=40 * 1024 * 1024
        ),
    )(queries, kv_rows, gate_totals, outgoing)


def outward_kernel(
    n_ep, product_ref, mixed_ref, heads_ref, result_ref,
    arrived, summed, crossed, final, h_sem, p_sem, r_sem, x_sem, ep_sem,
):
    own = lax.axis_index("ep")
    quarter = lax.axis_index("tp")
    across = lax.rem(quarter + 2, 4)
    beside = quarter + 1 - 2 * lax.rem(quarter, 2)
    diagonal = lax.rem(beside + 2, 4)
    meet((("ep", n_ep), ("tp", 4)))

    def heads_copy(step):
        place = lax.rem(quarter + step, 4)
        return pltpu.make_async_remote_copy(
            src_ref=mixed_ref.at[place],
            dst_ref=heads_ref.at[quarter],
            send_sem=h_sem.at[0, step],
            recv_sem=h_sem.at[1, step],
            device_id={"tp": place},
            device_id_type=pl.DeviceIdType.MESH,
        )

    def near(j):
        return push(product_ref.at[beside, j], arrived.at[0, j], p_sem, j, "tp", beside)

    def far(j):
        return push(product_ref.at[diagonal, j], arrived.at[1, j], r_sem, j, "tp", beside)

    def cross(j):
        return push(summed.at[j], crossed.at[j], x_sem, j, "tp", across)

    def home(j, source):
        return pltpu.make_async_remote_copy(
            src_ref=final.at[j],
            dst_ref=result_ref.at[source],
            send_sem=ep_sem.at[0, j],
            recv_sem=ep_sem.at[1, source],
            device_id={"ep": j},
            device_id_type=pl.DeviceIdType.MESH,
        )

    def begin(step, carry):
        j = lax.rem(own + step, n_ep)
        far(j).start()
        near(j).start()
        return carry

    lax.fori_loop(1, n_ep + 1, begin, 0)
    for step in range(1, 4):
        heads_copy(step).start()
    heads_ref[quarter] = mixed_ref[quarter]

    def pair_sum(step, carry):
        j = lax.rem(own + step, n_ep)
        far(j).wait_recv()
        total = product_ref[across, j].astype(jnp.float32) + arrived[1, j].astype(jnp.float32)
        summed[j] = total.astype(jnp.bfloat16)
        cross(j).start()
        return carry

    lax.fori_loop(1, n_ep + 1, pair_sum, 0)

    def finish(j):
        near(j).wait_recv()
        cross(j).wait_recv()
        total = product_ref[quarter, j].astype(jnp.float32) + arrived[0, j].astype(jnp.float32)
        return (total + crossed[j].astype(jnp.float32)).astype(jnp.bfloat16)

    def full_sum(step, carry):
        j = lax.rem(own + step, n_ep)
        final[j] = finish(j)
        home(j, own).start()
        return carry

    lax.fori_loop(1, n_ep, full_sum, 0)
    result_ref[own] = finish(own)
    for step in range(1, 4):
        heads_copy(step).wait()

    def drain(step, carry):
        j = lax.rem(own + step, n_ep)
        near(j).wait_send()
        far(j).wait_send()
        cross(j).wait_send()

        @pl.when(step < n_ep)
        def _():
            home(j, own).wait_send()
            home(j, j).wait_recv()

        return carry

    lax.fori_loop(1, n_ep + 1, drain, 0)


def outward(product, mixed):
    _, n_ep, slot_count, width = product.shape
    pair = pltpu.SemaphoreType.DMA((2, n_ep))
    chunk = (n_ep, slot_count, width)
    return pl.pallas_call(
        functools.partial(outward_kernel, n_ep),
        out_shape=(
            jax.ShapeDtypeStruct(mixed.shape, jnp.bfloat16),
            jax.ShapeDtypeStruct(chunk, jnp.bfloat16),
        ),
        in_specs=[pl.BlockSpec(memory_space=pltpu.VMEM)] * 2,
        out_specs=[pl.BlockSpec(memory_space=pltpu.VMEM)] * 2,
        scratch_shapes=[
            pltpu.VMEM((2,) + chunk, jnp.bfloat16),
            pltpu.VMEM(chunk, jnp.bfloat16),
            pltpu.VMEM(chunk, jnp.bfloat16),
            pltpu.VMEM(chunk, jnp.bfloat16),
            pltpu.SemaphoreType.DMA((2, 4)),
            pair, pair, pair, pair,
        ],
        compiler_params=pltpu.CompilerParams(
            collective_id=1, has_side_effects=True, vmem_limit_bytes=40 * 1024 * 1024
        ),
    )(product, mixed)


def attention_inputs(mixer_input, mixer_gain, w_query, w_key, w_value):
    row_count = mixer_input.shape[0]
    head_local = w_query.shape[1] // HD
    normed = norm_rows(mixer_input, mixer_gain).astype(jnp.bfloat16)
    w_kv = jnp.concatenate([w_key, w_value], axis=1)
    kv_rows = jnp.dot(normed, w_kv, preferred_element_type=jnp.float32).astype(jnp.bfloat16)
    queries = jnp.dot(normed, w_query, preferred_element_type=jnp.float32).astype(jnp.bfloat16)
    queries = queries * jnp.bfloat16(HD ** (-0.5))
    queries = jnp.transpose(queries.reshape(row_count, head_local, HD), (1, 0, 2))
    return queries, kv_rows


def routed_rows(expert_input, expert_ids, route_weight, expert_gain):
    row_count = expert_input.shape[0]
    quarters = lax.axis_size("tp")
    experts = lax.axis_size("ep")
    quarter_rows = row_count // quarters
    slot_count = 2 * TOP_K * quarter_rows // experts
    first = lax.axis_index("tp") * quarter_rows
    own_input = lax.dynamic_slice_in_dim(expert_input, first, quarter_rows, 0)
    own_weights = lax.dynamic_slice_in_dim(route_weight, first, quarter_rows, 0)
    routed = lax.dynamic_slice_in_dim(expert_ids, first, quarter_rows, 0)
    normed = norm_rows(own_input, expert_gain).astype(jnp.bfloat16)
    matches = routed[:, :, None] == jnp.arange(experts, dtype=jnp.int32)[None, None, :]
    matches = matches.astype(jnp.bfloat16)
    per_token = jnp.sum(matches, axis=1)
    position = jnp.arange(quarter_rows, dtype=jnp.int32)
    lower = (position[None, :] < position[:, None]).astype(jnp.bfloat16)
    before = jnp.dot(lower, per_token, preferred_element_type=jnp.float32)
    ranks = jnp.sum(matches.astype(jnp.float32) * before[:, None, :], axis=2).astype(jnp.int32)
    slots = routed * slot_count + ranks
    total_slots = experts * slot_count
    chosen = slots[:, :, None] == jnp.arange(total_slots, dtype=jnp.int32)[None, None, :]
    chosen = chosen.astype(jnp.bfloat16)
    outgoing = lax.dot_general(
        jnp.sum(chosen, axis=1), normed, (((0,), (0,)), ((), ())),
        preferred_element_type=jnp.float32,
    ).astype(jnp.bfloat16)
    return outgoing.reshape(experts, slot_count, -1), chosen, own_weights


def per_device(
    mixer_input,
    log_forget_total,
    mixer_gain,
    w_query,
    w_key,
    w_value,
    w_output,
    mixer_post_gain,
    expert_input,
    expert_ids,
    route_weight,
    expert_gain,
    w_gate,
    w_up,
    w_down,
    expert_post_gain,
):
    queries, kv_rows = attention_inputs(mixer_input, mixer_gain, w_query, w_key, w_value)
    outgoing, chosen, own_weights = routed_rows(
        expert_input, expert_ids, route_weight, expert_gain
    )
    mixed, slot_rows = inward(queries, kv_rows, log_forget_total, outgoing)
    flat_rows = slot_rows.reshape(-1, slot_rows.shape[-1])
    gate_part = jnp.dot(flat_rows, w_gate[0], preferred_element_type=jnp.float32)
    up_part = jnp.dot(flat_rows, w_up[0], preferred_element_type=jnp.float32)
    hidden = (jax.nn.silu(gate_part) * up_part).astype(jnp.bfloat16)
    product = jnp.dot(hidden, w_down[0], preferred_element_type=jnp.float32).astype(jnp.bfloat16)
    quarters = slot_rows.shape[0]
    heads, rows, _ = mixed.shape
    mixed_heads = jnp.transpose(mixed, (1, 0, 2)).reshape(quarters, rows // quarters, heads * HD)
    head_rows, returned = outward(product.reshape(slot_rows.shape), mixed_heads)
    by_rows = jnp.transpose(head_rows, (1, 0, 2)).reshape(rows // quarters, -1)
    projected = jnp.dot(by_rows, w_output, preferred_element_type=jnp.float32)
    mixer_out = norm_rows(projected, mixer_post_gain).astype(jnp.bfloat16)
    returned = returned.reshape(-1, returned.shape[-1])
    combined = 0.0
    for k in range(TOP_K):
        picked = jnp.dot(chosen[:, k], returned, preferred_element_type=jnp.float32)
        combined = combined + own_weights[:, k : k + 1] * picked
    expert_out = norm_rows(combined, expert_post_gain).astype(jnp.bfloat16)
    return (mixer_out, expert_out)


def solution(mesh):
    placed = (
        P("ep", None),
        P("tp", None),
        P(),
        P(None, "tp"),
        P(None, "tp"),
        P(None, "tp"),
        P(),
        P(),
        P("ep", None),
        P("ep", None),
        P("ep", None),
        P(),
        P("ep", None, "tp"),
        P("ep", None, "tp"),
        P("ep", "tp", None),
        P(),
    )
    return jax.shard_map(
        per_device,
        mesh=mesh,
        in_specs=placed,
        out_specs=(P(("ep", "tp"), None), P(("ep", "tp"), None)),
        check_vma=False,
    )
```
